32 devices in a mesh: dp: 4 (over y, x), kv: 4 (over z), tp: 2 (over core).
Axes of the slice: x: 2, y: 2, z: 4, core: 2. Of those that a mesh axis runs over, the one named last changes fastest.
Arguments:
- pieces: bfloat16 [4096, 8, 2048], P(('kv', 'tp'), 'dp'), parts along dimension 1, may hold values from -6 to 6
- new_tokens: bfloat16 [256, 2048], P(('dp', 'kv', 'tp')), parts along dimension 0, may hold values from -6 to 6
- w_query: bfloat16 [2048, 1024], P(None, 'tp'), may hold values from -0.125 to 0.125
- w_key: bfloat16 [2048, 1024], P(None, 'tp'), may hold values from -0.125 to 0.125
- w_value: bfloat16 [2048, 2048], P(None, 'tp'), may hold values from -0.125 to 0.125
- w_decay: bfloat16 [2048, 1024], P(None, 'tp'), may hold values from -0.125 to 0.125
- decay_bias: float32 [1024], replicated, may hold values from 0 to 9
- norm_gain: float32 [2048], replicated, may hold values from 0.1 to 1.9
- head_gain: float32 [2048], replicated, may hold values from 0.1 to 1.9
- w_out: bfloat16 [2048, 2048], replicated, may hold values from -0.125 to 0.125
- prompt_state: float32 [8, 8, 128, 256], P('dp', 'tp', 'kv'), parts along dimension 0, may hold values from -8 to 8
- decode_state: float32 [256, 8, 128, 256], P(('dp', 'kv'), 'tp'), parts along dimension 0, may hold values from -8 to 8
Outputs:
- mixed_piece: bfloat16 [4096, 8, 2048], P(('kv', 'tp'), 'dp'), parts along dimension 1
- mixed_decode: bfloat16 [256, 2048], P(('dp', 'kv', 'tp')), parts along dimension 0
- prompt_state_out: float32 [8, 8, 128, 256], P('dp', 'tp', 'kv'), parts along dimension 0
- decode_state_out: float32 [256, 8, 128, 256], P(('dp', 'kv'), 'tp'), parts along dimension 0
The draws below stay inside these ranges and needn't reach their ends.
There are 4 independent parts, one for each index of `dp`. The reference program is written for one: setup_inputs(seed, part) draws one part's arguments, and reference() takes and returns one part's arrays. A program takes and returns all parts, laid end to end along the dimension named above; an argument that names none is the same for every part. Nothing has to cross between parts.
All inputs are finite; a program needn't handle non-finite values.
Results may differ from the reference program's by a relative error of at most 0.014.
Values may be sent and summed in bfloat16 or wider, within the bound.
No kernel may reach another device: no remote copies, remote signals or barrier semaphores. Data moves between devices by JAX's collectives and lax.ppermute only.
A program may use at most 192 MiB of HBM per device.

```python
import jax
import jax.numpy as jnp
from jax import lax

D = 2048
HEADS = 8
DK = 128
DV = 256
BLOCK = 64
PROMPTS = 2
PIECE = 4096
DEC = 64


def block_scale(rng, extent, cuts, smallest, high):
    def one(axis_at, blocks):
        draws = jax.random.uniform(jax.random.fold_in(jax.random.fold_in(rng, 6), axis_at), (blocks,), jnp.float32, smallest / len(cuts), high / len(cuts))
        return jnp.repeat(jnp.exp(draws), extent[axis_at] // blocks).reshape((-1,) + (1,) * (len(extent) - axis_at - 1))

    level = one(*cuts[0])
    for cut in cuts[1:]:
        level = level * one(*cut)
    return level


def centred(rng, dims, spread, bound, cuts=(), held_as=jnp.bfloat16):
    values = spread * jax.random.normal(rng, dims, jnp.float32)
    if cuts:
        values = values * block_scale(rng, dims, cuts, -0.22, 0.18)
    return jnp.clip(values, -bound, bound).astype(held_as)


def setup_inputs(seed: int = 0, part: int = 0) -> dict:
    key_of = jax.random.split(jax.random.key(seed), 13)
    own_keys = jax.random.split(jax.random.fold_in(key_of[12], part), 13)
    return {
        "pieces": centred(own_keys[0], (PIECE, PROMPTS, D), 1.0, 6.0, ((0, 8),)),
        "new_tokens": centred(own_keys[1], (DEC, D), 1.0, 6.0, ((0, 8),)),
        "w_query": centred(key_of[2], (D, HEADS * DK), D ** -0.5, 0.125, ((1, 2),)),
        "w_key": centred(key_of[3], (D, HEADS * DK), D ** -0.5, 0.125, ((1, 2),)),
        "w_value": centred(key_of[4], (D, HEADS * DV), D ** -0.5, 0.125, ((1, 2),)),
        "w_decay": centred(key_of[5], (D, HEADS * DK), D ** -0.5, 0.125, ((1, 2),)),
        "decay_bias": jnp.clip(jax.random.uniform(key_of[6], (HEADS * DK,), jnp.float32, 0.0, 9.0), 0.0, 9.0),
        "norm_gain": jnp.clip(1.0 + 0.18 * jax.random.normal(key_of[7], (D,), jnp.float32), 0.1, 1.9),
        "head_gain": jnp.clip(1.0 + 0.18 * jax.random.normal(key_of[8], (HEADS * DV,), jnp.float32), 0.1, 1.9),
        "w_out": centred(key_of[9], (HEADS * DV, D), (HEADS * DV) ** -0.5, 0.125),
        "prompt_state": centred(own_keys[10], (PROMPTS, HEADS, DK, DV), 2.0, 8.0, ((1, 2), (2, 4)), jnp.float32),
        "decode_state": centred(own_keys[11], (DEC, HEADS, DK, DV), 2.0, 8.0, ((0, 4), (1, 2)), jnp.float32),
    }


highest = lax.Precision.HIGHEST
norm_eps = 0.1
decay_tau = 16.0
part_limit = 16

def rms_rows(row_block, gain):
    wide = row_block.astype(jnp.float32)
    factor = lax.rsqrt(lax.optimization_barrier(jnp.mean(wide * wide, axis=-1, keepdims=True)) + norm_eps)
    return (wide * factor * gain).astype(jnp.bfloat16)

def head_norm(outputs, gain):
    factor = lax.rsqrt(lax.optimization_barrier(jnp.mean(outputs * outputs, axis=-1, keepdims=True)) + norm_eps)
    flat = (outputs * factor).reshape(outputs.shape[:-2] + (-1,))
    return (flat * gain).astype(jnp.bfloat16)

def project_roles(row_block, w_query, w_key, w_value, w_decay, decay_bias):
    lead = row_block.shape[:-1]
    queries = (jnp.dot(row_block, w_query, preferred_element_type=jnp.float32) * DK ** (-0.5)).astype(jnp.bfloat16)
    keys_new = jnp.dot(row_block, w_key, preferred_element_type=jnp.float32).astype(jnp.bfloat16)
    values_new = jnp.dot(row_block, w_value, preferred_element_type=jnp.float32).astype(jnp.bfloat16)
    decays = jax.nn.log_sigmoid(jnp.dot(row_block, w_decay, preferred_element_type=jnp.float32) + decay_bias) / decay_tau
    return (queries.reshape(lead + (HEADS, DK)), keys_new.reshape(lead + (HEADS, DK)), values_new.reshape(lead + (HEADS, DV)), decays.reshape(lead + (HEADS, DK)))

def block_terms(q_blk, k_blk, v_blk, g_blk):
    block_len = q_blk.shape[0]
    part_len = min(part_limit, block_len)
    part_count = block_len // part_len
    within = jnp.cumsum(g_blk, axis=0)
    part_ends = within[part_len - 1::part_len]
    anchor = jnp.concatenate([jnp.zeros_like(part_ends[:1]), part_ends[:-1]], axis=0)
    q_wide = q_blk.astype(jnp.float32)
    k_wide = k_blk.astype(jnp.float32)
    q_parts = q_wide.reshape((part_count, part_len) + q_blk.shape[1:])
    w_parts = within.reshape((part_count, part_len) + within.shape[1:])
    near_query = (q_parts * jnp.exp(w_parts - anchor[:, None])).astype(jnp.bfloat16)
    near_key = (k_wide[None] * jnp.exp(anchor[:, None] - within[None])).astype(jnp.bfloat16)
    scores = jnp.einsum('itbhk,isbhk->ibhts', near_query, near_key, preferred_element_type=jnp.float32)
    row_pos = jnp.arange(part_count)[:, None] * part_len + jnp.arange(part_len)[None]
    keep = row_pos[:, :, None] >= jnp.arange(block_len)[None, None]
    weights = jnp.where(keep[:, None, None], scores, 0.0).astype(jnp.bfloat16)
    in_block = jnp.einsum('ibhts,sbhv->itbhv', weights, v_blk, preferred_element_type=jnp.float32)
    in_block = in_block.reshape((block_len,) + in_block.shape[2:])
    block_total = within[-1]
    start_query = (q_wide * jnp.exp(within)).astype(jnp.bfloat16)
    end_key = (k_wide * jnp.exp(block_total[None] - within)).astype(jnp.bfloat16)
    added = jnp.einsum('sbhk,sbhv->bhkv', end_key, v_blk, preferred_element_type=jnp.float32)
    return (in_block, start_query, block_total, added)

def block_attention(query_all, key_all, value_all, decay_all, start_states):
    seq_len = query_all.shape[0]
    block_count = seq_len // BLOCK

    def to_blocks(tensor):
        return tensor.reshape((block_count, BLOCK) + tensor.shape[1:])

    def advance(states, inputs):
        in_block, start_query, block_total, added = block_terms(*inputs)
        from_state = jnp.einsum('tbhk,bhkv->tbhv', start_query.astype(jnp.float32), states, precision=highest)
        carried = jnp.exp(block_total)[..., None] * states + added
        return (carried, from_state + in_block)
    final_states, outputs = lax.scan(advance, start_states, (to_blocks(query_all), to_blocks(key_all), to_blocks(value_all), to_blocks(decay_all)))
    return (outputs.reshape((seq_len,) + outputs.shape[2:]), final_states)

def single_token(query, key_new, value_new, decay, states):
    query = query.astype(jnp.float32)
    key_new = key_new.astype(jnp.float32)
    value_new = value_new.astype(jnp.float32)
    from_state = jnp.einsum('bhk,bhkv->bhv', query * jnp.exp(decay), states, precision=highest)
    token_score = lax.optimization_barrier(jnp.sum(query * key_new, axis=-1, keepdims=True))
    outputs = from_state + token_score * value_new
    carried = jnp.exp(decay)[..., None] * states + key_new[..., None] * value_new[..., None, :]
    return (outputs, carried)

def reference(pieces, new_tokens, w_query, w_key, w_value, w_decay, decay_bias, norm_gain, head_gain, w_out, prompt_state, decode_state):
    query_p, key_p, value_p, decay_p = project_roles(rms_rows(pieces, norm_gain), w_query, w_key, w_value, w_decay, decay_bias)
    piece_att, prompt_out = block_attention(query_p, key_p, value_p, decay_p, prompt_state)
    query_d, key_d, value_d, decay_d = project_roles(rms_rows(new_tokens, norm_gain), w_query, w_key, w_value, w_decay, decay_bias)
    decode_att, decode_out = single_token(query_d, key_d, value_d, decay_d, decode_state)
    mixed_piece = jnp.dot(head_norm(piece_att, head_gain), w_out, preferred_element_type=jnp.float32).astype(jnp.bfloat16)
    mixed_decode = jnp.dot(head_norm(decode_att, head_gain), w_out, preferred_element_type=jnp.float32).astype(jnp.bfloat16)
    return (mixed_piece, mixed_decode, prompt_out, decode_out)
```

```python
import jax
import jax.numpy as jnp
from jax import lax
from jax.experimental import pallas as pl
from jax.experimental.pallas import tpu as pltpu
from jax.sharding import PartitionSpec as P

DK = 128
DV = 256
BLOCK = 64


highest = lax.Precision.HIGHEST
norm_eps = 0.1
decay_tau = 16.0
part_limit = 16


def rms_rows(row_block, gain):
    wide = row_block.astype(jnp.float32)
    factor = lax.rsqrt(jnp.mean(wide * wide, axis=-1, keepdims=True) + norm_eps)
    return (wide * factor * gain).astype(jnp.bfloat16)


def head_norm(outputs, gain):
    factor = lax.rsqrt(jnp.mean(outputs * outputs, axis=-1, keepdims=True) + norm_eps)
    flat = (outputs * factor).reshape(outputs.shape[:-2] + (-1,))
    return (flat * gain).astype(jnp.bfloat16)


def single_token(query, key_new, value_new, decay, states):
    query = query.astype(jnp.float32)
    key_new = key_new.astype(jnp.float32)
    value_new = value_new.astype(jnp.float32)
    from_state = jnp.einsum("bhk,bhkv->bhv", query * jnp.exp(decay), states, precision=highest)
    token_score = jnp.sum(query * key_new, axis=-1, keepdims=True)
    outputs = from_state + token_score * value_new
    carried = jnp.exp(decay)[..., None] * states + key_new[..., None] * value_new[..., None, :]
    return (outputs, carried)


NT = (((1,), (1,)), ((), ()))
TN = (((0,), (0,)), ((), ()))


def split_sum(selector, wide):
    high = wide.astype(jnp.bfloat16)
    rest = wide - high.astype(jnp.float32)
    middle = rest.astype(jnp.bfloat16)
    low = (rest - middle.astype(jnp.float32)).astype(jnp.bfloat16)
    dot = lambda part: jnp.dot(selector, part, preferred_element_type=jnp.float32)
    return dot(high) + (dot(middle) + dot(low))


def as_column(row):
    return jnp.transpose(jnp.broadcast_to(row, (8, row.shape[1])))[:, :1]


def positions(shape, axis):
    return lax.broadcasted_iota(jnp.int32, shape, axis)


def local_state_kernel(k_ref, v_ref, g_ref, state_ref, total_ref):
    rows = k_ref.shape[1]
    heads = k_ref.shape[2] // DK

    @pl.when(pl.program_id(1) == 0)
    def _():
        state_ref[...] = jnp.zeros_like(state_ref)
        total_ref[...] = jnp.zeros_like(total_ref)

    decay = g_ref[0]
    later = (positions((rows, rows), 1) > positions((rows, rows), 0)).astype(jnp.bfloat16)
    after = split_sum(later, decay)
    total = after[:1] + decay[:1]
    end_key = (k_ref[0].astype(jnp.float32) * jnp.exp(after)).astype(jnp.bfloat16)
    for head in range(heads):
        ks = slice(head * DK, (head + 1) * DK)
        vs = slice(head * DV, (head + 1) * DV)
        added = lax.dot_general(
            end_key[:, ks], v_ref[0, :, vs], TN, preferred_element_type=jnp.float32
        )
        state_ref[0, head] = as_column(jnp.exp(total[:, ks])) * state_ref[0, head] + added
    total_ref[0] = total_ref[0] + total


def attention_kernel(q_ref, k_ref, v_ref, g_ref, start_ref, gain_ref, out_ref, state_ref):
    rows = q_ref.shape[1]
    heads = q_ref.shape[2] // DK
    parts = BLOCK // part_limit

    @pl.when(pl.program_id(1) == 0)
    def _():
        state_ref[...] = start_ref[0]

    t_pos = positions((rows, rows), 0)
    s_pos = positions((rows, rows), 1)
    same_part = (t_pos // part_limit == s_pos // part_limit) & (s_pos <= t_pos)
    near_all = split_sum(same_part.astype(jnp.bfloat16), g_ref[0])
    row_t = positions((BLOCK, parts * BLOCK), 0)
    col = positions((BLOCK, parts * BLOCK), 1)
    keep = (row_t // part_limit == col // BLOCK) & (col % BLOCK <= row_t)
    for block in range(rows // BLOCK):
        at = slice(block * BLOCK, (block + 1) * BLOCK)
        near = near_all[at]
        q_wide = q_ref[0, at].astype(jnp.float32)
        k_wide = k_ref[0, at].astype(jnp.float32)
        v_blk = v_ref[0, at]
        anchors = [jnp.zeros_like(near[:1])]
        for part in range(parts):
            last = (part + 1) * part_limit - 1
            anchors.append(anchors[-1] + near[last : last + 1])
        total = anchors[-1]
        within = jnp.concatenate(
            [
                near[part * part_limit : (part + 1) * part_limit] + anchors[part]
                for part in range(parts)
            ],
            axis=0,
        )
        near_query = (q_wide * jnp.exp(near)).astype(jnp.bfloat16)
        near_key = jnp.concatenate(
            [k_wide * jnp.exp(anchors[part] - within) for part in range(parts)], axis=0
        ).astype(jnp.bfloat16)
        start_query = (q_wide * jnp.exp(within)).astype(jnp.bfloat16)
        end_key = (k_wide * jnp.exp(total - within)).astype(jnp.bfloat16)
        kept = jnp.exp(total)
        for head in range(heads):
            ks = slice(head * DK, (head + 1) * DK)
            vs = slice(head * DV, (head + 1) * DV)
            v_head = v_blk[:, vs]
            scores = lax.dot_general(
                near_query[:, ks], near_key[:, ks], NT, preferred_element_type=jnp.float32
            )
            weights = jnp.where(keep, scores, 0.0).astype(jnp.bfloat16)
            state = state_ref[head]
            att = jnp.dot(
                weights,
                jnp.concatenate([v_head] * parts, axis=0),
                preferred_element_type=jnp.float32,
            ) + jnp.dot(
                start_query[:, ks], state.astype(jnp.bfloat16), preferred_element_type=jnp.float32
            )
            added = lax.dot_general(end_key[:, ks], v_head, TN, preferred_element_type=jnp.float32)
            state_ref[head] = as_column(kept[:, ks]) * state + added
            factor = lax.rsqrt(jnp.mean(att * att, axis=-1, keepdims=True) + norm_eps)
            out_ref[0, at, vs] = (att * factor * gain_ref[:, vs]).astype(jnp.bfloat16)


def hand_on(values, axis):
    count = lax.axis_size(axis)
    return lax.ppermute(values, axis, [(at, at + 1) for at in range(count - 1)])


def on_device(
    pieces,
    new_tokens,
    w_query,
    w_key,
    w_value,
    w_decay,
    decay_bias,
    norm_gain,
    head_gain,
    w_out,
    prompt_state,
    decode_state,
):
    tp_size = lax.axis_size("tp")
    kv_size = lax.axis_size("kv")
    tp_index = lax.axis_index("tp")
    kv_index = lax.axis_index("kv")
    heads = w_query.shape[1] // DK
    bias_here = lax.dynamic_slice_in_dim(decay_bias, tp_index * (heads * DK), heads * DK)
    gain_here = lax.dynamic_slice_in_dim(head_gain, tp_index * (heads * DV), heads * DV)
    own_pos, prompt_count, width = pieces.shape
    piece_count = own_pos * prompt_count
    whole_start = lax.all_gather(prompt_state.astype(jnp.bfloat16), "kv", axis=2, tiled=True)
    normed_piece = rms_rows(pieces, norm_gain).transpose(1, 0, 2).reshape(piece_count, width)
    rows_all = jnp.concatenate([normed_piece, rms_rows(new_tokens, norm_gain)], axis=0)
    row_count = rows_all.shape[0]
    dec_count = row_count - piece_count
    row_block = lax.all_gather(rows_all, "tp", axis=0, tiled=True)

    def project(weight):
        return jnp.dot(row_block, weight, preferred_element_type=jnp.float32)

    by_owner = lambda value: value.reshape(tp_size, row_count, value.shape[-1])
    keys = by_owner(project(w_key).astype(jnp.bfloat16))
    values = by_owner(project(w_value).astype(jnp.bfloat16))
    decays = by_owner(jax.nn.log_sigmoid(project(w_decay) + bias_here) / decay_tau)
    queries = by_owner((project(w_query) * DK ** (-0.5)).astype(jnp.bfloat16))

    def row_spec(step, columns):
        per_owner = own_pos // step

        def where(prompt, at):
            return (at // per_owner, prompt * per_owner + at % per_owner, 0)

        return pl.BlockSpec((1, step, columns), where)

    step = 2 * BLOCK if own_pos % (2 * BLOCK) == 0 else BLOCK
    steps = tp_size * own_pos // step
    order = pltpu.CompilerParams(dimension_semantics=("arbitrary", "arbitrary"))
    state_spec = pl.BlockSpec((1, heads, DK, DV), lambda prompt, at: (prompt, 0, 0, 0))
    local_states, totals = pl.pallas_call(
        local_state_kernel,
        grid=(prompt_count, steps),
        in_specs=[row_spec(step, heads * DK), row_spec(step, heads * DV), row_spec(step, heads * DK)],
        out_specs=[state_spec, pl.BlockSpec((1, 1, heads * DK), lambda prompt, at: (prompt, 0, 0))],
        out_shape=[
            jax.ShapeDtypeStruct((prompt_count, heads, DK, DV), jnp.float32),
            jax.ShapeDtypeStruct((prompt_count, 1, heads * DK), jnp.float32),
        ],
        compiler_params=order,
        name="local_state",
    )(keys, values, decays)
    kept = jnp.exp(totals).reshape(prompt_count, heads, DK)[..., None]
    incoming = [whole_start[at].astype(jnp.float32) for at in range(prompt_count)]
    for hop in range(kv_size - 1):
        for at in range(prompt_count):
            leaving = (kept[at] * incoming[at] + local_states[at]).astype(jnp.bfloat16)
            arrived = hand_on(leaving, "kv").astype(jnp.float32)
            incoming[at] = jnp.where(kv_index == hop + 1, arrived, incoming[at])
    incoming = jnp.stack(incoming)
    send_rows = pl.pallas_call(
        attention_kernel,
        grid=(prompt_count, steps),
        in_specs=[
            row_spec(step, heads * DK),
            row_spec(step, heads * DK),
            row_spec(step, heads * DV),
            row_spec(step, heads * DK),
            state_spec,
            pl.BlockSpec((1, heads * DV), lambda prompt, at: (0, 0)),
        ],
        out_specs=row_spec(step, heads * DV),
        out_shape=jax.ShapeDtypeStruct((tp_size, row_count, heads * DV), jnp.bfloat16),
        scratch_shapes=[pltpu.VMEM((heads, DK, DV), jnp.float32)],
        compiler_params=order,
        name="attention",
    )(queries, keys, values, decays, incoming, gain_here[None])
    final_all = (kept * incoming + local_states).astype(jnp.bfloat16)
    rows_k = prompt_state.shape[2]
    last = kv_size - 1
    slices = [final_all[:, :, at * rows_k : (at + 1) * rows_k] for at in range(kv_size)]
    prompt_out = slices[last]
    for at in range(last):
        arrived = lax.ppermute(slices[at], "kv", [(last, at)])
        prompt_out = jnp.where(kv_index == at, arrived, prompt_out)
    prompt_out = prompt_out.astype(jnp.float32)

    def decode_rows(value, columns):
        picked = value[:, piece_count:].reshape(tp_size * dec_count, heads, columns)
        return picked

    decode_att, decode_out = single_token(
        decode_rows(queries, DK),
        decode_rows(keys, DK),
        decode_rows(values, DV),
        decode_rows(decays, DK),
        decode_state,
    )
    dec_normed = head_norm(decode_att, gain_here).reshape(tp_size, dec_count, heads * DV)
    send_rows = lax.dynamic_update_slice(send_rows, dec_normed, (0, piece_count, 0))
    mixed = jnp.dot(
        lax.all_to_all(send_rows, "tp", split_axis=0, concat_axis=2, tiled=True)[0],
        w_out,
        preferred_element_type=jnp.float32,
    ).astype(jnp.bfloat16)
    mixed_piece = mixed[:piece_count].reshape(prompt_count, own_pos, width).transpose(1, 0, 2)
    return (mixed_piece, mixed[piece_count:], prompt_out, decode_out)


def solution(mesh):
    return jax.shard_map(
        on_device,
        mesh=mesh,
        in_specs=(
            P(("kv", "tp"), "dp", None),
            P(("dp", "kv", "tp"), None),
            P(None, "tp"),
            P(None, "tp"),
            P(None, "tp"),
            P(None, "tp"),
            P(),
            P(),
            P(),
            P(),
            P("dp", "tp", "kv", None),
            P(("dp", "kv"), "tp", None, None),
        ),
        out_specs=(
            P(("kv", "tp"), "dp", None),
            P(("dp", "kv", "tp"), None),
            P("dp", "tp", "kv", None),
            P(("dp", "kv"), "tp", None, None),
        ),
        check_vma=False,
    )
```

```python
import jax
import jax.numpy as jnp
from jax import lax
from jax.experimental import pallas as pl
from jax.experimental.pallas import tpu as pltpu
from jax.sharding import PartitionSpec as P

DK = 128
DV = 256
BLOCK = 64


highest = lax.Precision.HIGHEST
norm_eps = 0.1
decay_tau = 16.0
part_limit = 16


def rms_rows(row_block, gain):
    wide = row_block.astype(jnp.float32)
    factor = lax.rsqrt(jnp.mean(wide * wide, axis=-1, keepdims=True) + norm_eps)
    return (wide * factor * gain).astype(jnp.bfloat16)


def head_norm(outputs, gain):
    factor = lax.rsqrt(jnp.mean(outputs * outputs, axis=-1, keepdims=True) + norm_eps)
    flat = (outputs * factor).reshape(outputs.shape[:-2] + (-1,))
    return (flat * gain).astype(jnp.bfloat16)


def single_token(query, key_new, value_new, decay, states):
    query = query.astype(jnp.float32)
    key_new = key_new.astype(jnp.float32)
    value_new = value_new.astype(jnp.float32)
    from_state = jnp.einsum("bhk,bhkv->bhv", query * jnp.exp(decay), states, precision=highest)
    token_score = jnp.sum(query * key_new, axis=-1, keepdims=True)
    outputs = from_state + token_score * value_new
    carried = jnp.exp(decay)[..., None] * states + key_new[..., None] * value_new[..., None, :]
    return (outputs, carried)


NT = (((1,), (1,)), ((), ()))
TN = (((0,), (0,)), ((), ()))


def split_sum(selector, wide):
    high = wide.astype(jnp.bfloat16)
    rest = wide - high.astype(jnp.float32)
    middle = rest.astype(jnp.bfloat16)
    low = (rest - middle.astype(jnp.float32)).astype(jnp.bfloat16)
    dot = lambda part: jnp.dot(selector, part, preferred_element_type=jnp.float32)
    return dot(high) + (dot(middle) + dot(low))


def as_column(row):
    return jnp.transpose(jnp.broadcast_to(row, (8, row.shape[1])))[:, :1]


def positions(shape, axis):
    return lax.broadcasted_iota(jnp.int32, shape, axis)


def local_state_kernel(k_ref, v_ref, g_ref, state_ref, total_ref):
    rows = k_ref.shape[1]
    heads = k_ref.shape[2] // DK

    @pl.when(pl.program_id(1) == 0)
    def _():
        state_ref[...] = jnp.zeros_like(state_ref)
        total_ref[...] = jnp.zeros_like(total_ref)

    decay = g_ref[0]
    later = (positions((rows, rows), 1) > positions((rows, rows), 0)).astype(jnp.bfloat16)
    after = split_sum(later, decay)
    total = after[:1] + decay[:1]
    end_key = (k_ref[0].astype(jnp.float32) * jnp.exp(after)).astype(jnp.bfloat16)
    for head in range(heads):
        ks = slice(head * DK, (head + 1) * DK)
        vs = slice(head * DV, (head + 1) * DV)
        added = lax.dot_general(
            end_key[:, ks], v_ref[0, :, vs], TN, preferred_element_type=jnp.float32
        )
        state_ref[0, head] = as_column(jnp.exp(total[:, ks])) * state_ref[0, head] + added
    total_ref[0] = total_ref[0] + total


def attention_kernel(q_ref, k_ref, v_ref, g_ref, start_ref, gain_ref, out_ref, state_ref):
    rows = q_ref.shape[1]
    heads = q_ref.shape[2] // DK
    parts = BLOCK // part_limit

    @pl.when(pl.program_id(1) == 0)
    def _():
        state_ref[...] = start_ref[0]

    t_pos = positions((rows, rows), 0)
    s_pos = positions((rows, rows), 1)
    same_part = (t_pos // part_limit == s_pos // part_limit) & (s_pos <= t_pos)
    near_all = split_sum(same_part.astype(jnp.bfloat16), g_ref[0])
    row_t = positions((BLOCK, parts * BLOCK), 0)
    col = positions((BLOCK, parts * BLOCK), 1)
    keep = (row_t // part_limit == col // BLOCK) & (col % BLOCK <= row_t)
    for block in range(rows // BLOCK):
        at = slice(block * BLOCK, (block + 1) * BLOCK)
        near = near_all[at]
        q_wide = q_ref[0, at].astype(jnp.float32)
        k_wide = k_ref[0, at].astype(jnp.float32)
        v_blk = v_ref[0, at]
        anchors = [jnp.zeros_like(near[:1])]
        for part in range(parts):
            last = (part + 1) * part_limit - 1
            anchors.append(anchors[-1] + near[last : last + 1])
        total = anchors[-1]
        within = jnp.concatenate(
            [
                near[part * part_limit : (part + 1) * part_limit] + anchors[part]
                for part in range(parts)
            ],
            axis=0,
        )
        near_query = (q_wide * jnp.exp(near)).astype(jnp.bfloat16)
        near_key = jnp.concatenate(
            [k_wide * jnp.exp(anchors[part] - within) for part in range(parts)], axis=0
        ).astype(jnp.bfloat16)
        start_query = (q_wide * jnp.exp(within)).astype(jnp.bfloat16)
        end_key = (k_wide * jnp.exp(total - within)).astype(jnp.bfloat16)
        kept = jnp.exp(total)
        for head in range(heads):
            ks = slice(head * DK, (head + 1) * DK)
            vs = slice(head * DV, (head + 1) * DV)
            v_head = v_blk[:, vs]
            scores = lax.dot_general(
                near_query[:, ks], near_key[:, ks], NT, preferred_element_type=jnp.float32
            )
            weights = jnp.where(keep, scores, 0.0).astype(jnp.bfloat16)
            state = state_ref[head]
            att = jnp.dot(
                weights,
                jnp.concatenate([v_head] * parts, axis=0),
                preferred_element_type=jnp.float32,
            ) + jnp.dot(
                start_query[:, ks], state.astype(jnp.bfloat16), preferred_element_type=jnp.float32
            )
            added = lax.dot_general(end_key[:, ks], v_head, TN, preferred_element_type=jnp.float32)
            state_ref[head] = as_column(kept[:, ks]) * state + added
            factor = lax.rsqrt(jnp.mean(att * att, axis=-1, keepdims=True) + norm_eps)
            out_ref[0, at, vs] = (att * factor * gain_ref[:, vs]).astype(jnp.bfloat16)


def hand_on(values, axis):
    count = lax.axis_size(axis)
    return lax.ppermute(values, axis, [(at, at + 1) for at in range(count - 1)])


def on_device(
    pieces,
    new_tokens,
    w_query,
    w_key,
    w_value,
    w_decay,
    decay_bias,
    norm_gain,
    head_gain,
    w_out,
    prompt_state,
    decode_state,
):
    tp_size = lax.axis_size("tp")
    kv_size = lax.axis_size("kv")
    tp_index = lax.axis_index("tp")
    kv_index = lax.axis_index("kv")
    heads = w_query.shape[1] // DK
    bias_here = lax.dynamic_slice_in_dim(decay_bias, tp_index * (heads * DK), heads * DK)
    gain_here = lax.dynamic_slice_in_dim(head_gain, tp_index * (heads * DV), heads * DV)
    own_pos, prompt_count, width = pieces.shape
    piece_count = own_pos * prompt_count
    own_start = prompt_state.astype(jnp.bfloat16)
    whole_start = jnp.concatenate(
        [own_start] + [lax.ppermute(own_start, "kv", [(at, 0)]) for at in range(1, kv_size)], axis=2
    )
    normed_piece = rms_rows(pieces, norm_gain).transpose(1, 0, 2).reshape(piece_count, width)
    rows_all = jnp.concatenate([normed_piece, rms_rows(new_tokens, norm_gain)], axis=0)
    row_count = rows_all.shape[0]
    dec_count = row_count - piece_count
    by_shift = [rows_all] + [
        lax.ppermute(rows_all, "tp", [(at, (at + shift) % tp_size) for at in range(tp_size)])
        for shift in range(1, tp_size)
    ]
    by_index = []
    for owner in range(tp_size):
        picked = by_shift[0]
        for shift in range(1, tp_size):
            picked = jnp.where((tp_index - owner) % tp_size == shift, by_shift[shift], picked)
        by_index.append(picked)
    row_block = jnp.concatenate(by_index, axis=0)

    def project(weight):
        return jnp.dot(row_block, weight, preferred_element_type=jnp.float32)

    by_owner = lambda value: value.reshape(tp_size, row_count, value.shape[-1])
    keys = by_owner(project(w_key).astype(jnp.bfloat16))
    values = by_owner(project(w_value).astype(jnp.bfloat16))
    decays = by_owner(jax.nn.log_sigmoid(project(w_decay) + bias_here) / decay_tau)
    queries = by_owner((project(w_query) * DK ** (-0.5)).astype(jnp.bfloat16))

    def row_spec(step, columns):
        per_owner = own_pos // step

        def where(prompt, at):
            return (at // per_owner, prompt * per_owner + at % per_owner, 0)

        return pl.BlockSpec((1, step, columns), where)

    step = 2 * BLOCK if own_pos % (2 * BLOCK) == 0 else BLOCK
    steps = tp_size * own_pos // step
    order = pltpu.CompilerParams(dimension_semantics=("arbitrary", "arbitrary"))
    state_spec = pl.BlockSpec((1, heads, DK, DV), lambda prompt, at: (prompt, 0, 0, 0))
    local_states, totals = pl.pallas_call(
        local_state_kernel,
        grid=(prompt_count, steps),
        in_specs=[row_spec(step, heads * DK), row_spec(step, heads * DV), row_spec(step, heads * DK)],
        out_specs=[state_spec, pl.BlockSpec((1, 1, heads * DK), lambda prompt, at: (prompt, 0, 0))],
        out_shape=[
            jax.ShapeDtypeStruct((prompt_count, heads, DK, DV), jnp.float32),
            jax.ShapeDtypeStruct((prompt_count, 1, heads * DK), jnp.float32),
        ],
        compiler_params=order,
        name="local_state",
    )(keys, values, decays)
    kept = jnp.exp(totals).reshape(prompt_count, heads, DK)[..., None]
    incoming = [whole_start[at].astype(jnp.float32) for at in range(prompt_count)]
    for hop in range(kv_size - 1):
        for at in range(prompt_count):
            leaving = (kept[at] * incoming[at] + local_states[at]).astype(jnp.bfloat16)
            arrived = hand_on(leaving, "kv").astype(jnp.float32)
            incoming[at] = jnp.where(kv_index == hop + 1, arrived, incoming[at])
    incoming = jnp.stack(incoming)
    send_rows = pl.pallas_call(
        attention_kernel,
        grid=(prompt_count, steps),
        in_specs=[
            row_spec(step, heads * DK),
            row_spec(step, heads * DK),
            row_spec(step, heads * DV),
            row_spec(step, heads * DK),
            state_spec,
            pl.BlockSpec((1, heads * DV), lambda prompt, at: (0, 0)),
        ],
        out_specs=row_spec(step, heads * DV),
        out_shape=jax.ShapeDtypeStruct((tp_size, row_count, heads * DV), jnp.bfloat16),
        scratch_shapes=[pltpu.VMEM((heads, DK, DV), jnp.float32)],
        compiler_params=order,
        name="attention",
    )(queries, keys, values, decays, incoming, gain_here[None])
    final_all = (kept * incoming + local_states).astype(jnp.bfloat16)
    rows_k = prompt_state.shape[2]
    last = kv_size - 1
    slices = [final_all[:, :, at * rows_k : (at + 1) * rows_k] for at in range(kv_size)]
    prompt_out = slices[last]
    for at in range(last):
        arrived = lax.ppermute(slices[at], "kv", [(last, at)])
        prompt_out = jnp.where(kv_index == at, arrived, prompt_out)
    prompt_out = prompt_out.astype(jnp.float32)

    def decode_rows(value, columns):
        picked = value[:, piece_count:].reshape(tp_size * dec_count, heads, columns)
        return picked

    decode_att, decode_out = single_token(
        decode_rows(queries, DK),
        decode_rows(keys, DK),
        decode_rows(values, DV),
        decode_rows(decays, DK),
        decode_state,
    )
    dec_normed = head_norm(decode_att, gain_here).reshape(tp_size, dec_count, heads * DV)
    send_rows = lax.dynamic_update_slice(send_rows, dec_normed, (0, piece_count, 0))
    own_rows = lax.all_to_all(send_rows, "tp", split_axis=0, concat_axis=0, tiled=True)
    columns = heads * DV
    mixed = sum(
        jnp.dot(
            own_rows[at],
            w_out[at * columns : (at + 1) * columns],
            preferred_element_type=jnp.float32,
        )
        for at in range(tp_size)
    ).astype(jnp.bfloat16)
    mixed_piece = mixed[:piece_count].reshape(prompt_count, own_pos, width).transpose(1, 0, 2)
    return (mixed_piece, mixed[piece_count:], prompt_out, decode_out)


def solution(mesh):
    return jax.shard_map(
        on_device,
        mesh=mesh,
        in_specs=(
            P(("kv", "tp"), "dp", None),
            P(("dp", "kv", "tp"), None),
            P(None, "tp"),
            P(None, "tp"),
            P(None, "tp"),
            P(None, "tp"),
            P(),
            P(),
            P(),
            P(),
            P("dp", "tp", "kv", None),
            P(("dp", "kv"), "tp", None, None),
        ),
        out_specs=(
            P(("kv", "tp"), "dp", None),
            P(("dp", "kv", "tp"), None),
            P("dp", "tp", "kv", None),
            P(("dp", "kv"), "tp", None, None),
        ),
        check_vma=False,
    )
```
